32 devices in a mesh: ep: 16 (over z, y, x), tp: 2 (over core).
Axes of the slice: x: 2, y: 2, z: 4, core: 2. Of those that a mesh axis runs over, the one named last changes fastest.
Arguments:
- tokens: bfloat16 [512, 2048], P('ep'), may hold values from -6 to 6
- lengths: int32 [512], P('ep'), may hold values from 128 to 1024
- key_cache: bfloat16 [512, 1024, 256], P('ep', None, 'tp'), may hold values from -1000 to 1000
- value_cache: bfloat16 [512, 1024, 256], P('ep', None, 'tp'), may hold values from -6 to 6
- gate_cache: float32 [512, 16, 1024], P('ep', 'tp'), may hold values from -130 to 0, as said below
- mix_gain: float32 [2048], replicated, may hold values from 0.1 to 1.9
- query_weight: bfloat16 [2048, 1024], P(None, 'tp'), may hold values from -0.125 to 0.125
- key_weight: bfloat16 [2048, 256], P(None, 'tp'), may hold values from -0.125 to 0.125
- value_weight: bfloat16 [2048, 256], P(None, 'tp'), may hold values from -0.125 to 0.125
- forget_weight: bfloat16 [2048, 16], P(None, 'tp'), may hold values from -0.125 to 0.125
- out_weight: bfloat16 [1024, 2048], P('tp'), may hold values from -0.1875 to 0.1875
- expert_gain: float32 [2048], replicated, may hold values from 0.1 to 1.9
- routes: int32 [512, 2], P('ep'), may hold values from 0 to 7, all different within a row; in each aligned block of 32 rows (0 to 31, 32 to 63, ...) at most 12 rows name the same one
- route_weights: float32 [512, 2], P('ep'), may hold values from 0.2 to 1
- expert_gate: bfloat16 [2048, 65536], P(None, ('ep', 'tp')), may hold values from -0.125 to 0.125
- expert_up: bfloat16 [2048, 65536], P(None, ('ep', 'tp')), may hold values from -0.125 to 0.125
- expert_down: bfloat16 [65536, 2048], P(('ep', 'tp')), may hold values from -0.0625 to 0.0625
Outputs:
- layer_out: bfloat16 [512, 2048], P('ep')
The draws below stay inside these ranges and needn't reach their ends.
Inputs may be any that keep to these rules, and one draw needn't show every extreme that they name: `routes`: within the rows of one index of ep, no expert is named more than 12 times, and in every draw some expert is named exactly 12 times in some such rows; the 2 experts of a row differ. `gate_cache`: for each sequence and head the values never rise along the cache positions.
All inputs are finite; a program needn't handle non-finite values.
Results may differ from the reference program's by a relative error of at most 0.013.
Values may be sent and summed in bfloat16 or wider, within the bound.
No kernel may reach another device: no remote copies, remote signals or barrier semaphores. Data moves between devices by JAX's collectives and lax.ppermute only.
A program may use at most 128 MiB of HBM per device.

```python
import math
import jax
import jax.numpy as jnp
import numpy as np
from jax import lax

D = 2048
HEADS = 16
KV_HEADS = 4
HD = 64
FF = 8192
EXPERTS = 8
TOP = 2
SEQ_DEV = 32
CACHE_POSITIONS = 1024
CAP = 12
SEQUENCE_TOTAL = 512
N_EP = 16
N_TP = 2


def draw_gate_cache(key, part):
    key_fragments = jax.random.split(jax.random.fold_in(key, 11), 7)
    order = jax.random.permutation(key_fragments[0], HEADS)
    slow = order < HEADS // 2
    slow_rate = jax.random.uniform(key_fragments[1], (SEQUENCE_TOTAL, HEADS), jnp.float32, 0.1, 0.5) / CACHE_POSITIONS
    fast_rate = jnp.exp(jax.random.uniform(key_fragments[2], (SEQUENCE_TOTAL, HEADS), jnp.float32, jnp.log(1.0 / 100.0), jnp.log(1.0 / 30.0)))
    rate = jnp.where(slow[None, :], slow_rate, fast_rate)
    seq_factor = jnp.exp(jax.random.uniform(key_fragments[3], (SEQUENCE_TOTAL, 1, 1), jnp.float32, -0.7, 0.7))
    rough = jax.random.uniform(key_fragments[4], (SEQUENCE_TOTAL, HEADS, CACHE_POSITIONS), jnp.float32, 0.4, 1.6)
    step_log_gates = -rate[:, :, None] * seq_factor * rough
    spike_position = jax.random.randint(key_fragments[5], (SEQUENCE_TOTAL, 3), 0, CACHE_POSITIONS)
    decay_amounts = jax.random.uniform(key_fragments[6], (SEQUENCE_TOTAL, 3), jnp.float32, 0.2, 0.4)
    cache_locations = jnp.arange(CACHE_POSITIONS, dtype=jnp.int32)
    spike_events = jnp.sum(jnp.where(cache_locations[None, None, :] == spike_position[:, :, None], jnp.log(1.0 - decay_amounts)[:, :, None], 0.0), axis=1)
    step_log_gates = step_log_gates + spike_events[:, None, :]
    return jnp.cumsum(step_log_gates, axis=-1).astype(jnp.float32)


def draw_key_cache(key, part):
    key_fragments = jax.random.split(jax.random.fold_in(key, 23), 1)
    base = jnp.clip(jax.random.normal(key_fragments[0], (SEQUENCE_TOTAL, CACHE_POSITIONS, KV_HEADS * HD), jnp.float32), -6.0, 6.0)
    return base.astype(jnp.bfloat16)


def with_ends(values, rng, smallest, largest):
    shape = values.shape
    place = [jax.random.randint(jax.random.fold_in(rng, axis), (), 0, shape[axis]) for axis in range(len(shape))]
    values = values.at[tuple(place)].set(smallest)
    longest = shape.index(max(shape))
    place[longest] = (place[longest] + 1) % shape[longest]
    return values.at[tuple(place)].set(largest)


def levels(rng, dims, cuts, smallest, top_value):
    level = 1.0
    for axis_at, shards_of in cuts:
        steps = jax.random.uniform(jax.random.fold_in(jax.random.fold_in(rng, 6), axis_at), (shards_of,), jnp.float32, smallest / len(cuts), top_value / len(cuts))
        level = level * jnp.repeat(jnp.exp(steps), dims[axis_at] // shards_of).reshape((-1,) + (1,) * (len(dims) - 1 - axis_at))
    return level


def deal_out(key, own, number, rows, count, top, bound, lean):
    sequence = jax.random.permutation(key, count)
    crowded, usual = shares(count, rows * top, bound, lean, True), shares(count, rows * top, bound, lean, False)
    places = jnp.arange(count)

    def named(sizes, rotation):
        used = int((sizes > 0).sum())
        fixed = max(1, used // 4)
        shifted = fixed + (places - fixed + rotation * (used - fixed)) % max(1, count - fixed)
        return jnp.zeros((count,), jnp.int32).at[sequence[jnp.where(places < fixed, places, shifted)]].set(jnp.asarray(sizes, jnp.int32))

    sizes = jnp.where(number % 4 == 0, named(crowded, number // 4), named(usual, number - number // 4 - 1))
    mixed = jax.random.permutation(jax.random.fold_in(own, 3), count)
    source_of, taker = mixed[0:count // 2 * 2:2], mixed[1:count // 2 * 2:2]
    room = jnp.minimum(sizes[source_of] - 1, bound - sizes[taker]) // 2
    room = jnp.where((source_of == sequence[0]) | (taker == sequence[0]) | (sizes[taker] == 0), 0, jnp.maximum(room, 0))
    shifted = jax.random.randint(jax.random.fold_in(own, 4), (count // 2,), 0, 1 << 20) % (room + 1)
    sizes = sizes.at[source_of].add(-shifted).at[taker].add(shifted)
    members = jnp.searchsorted(jnp.cumsum(sizes), jnp.arange(rows * top), side="right").astype(jnp.int32)
    listing = members.reshape(top, rows).T
    listing = listing[jax.random.permutation(jax.random.fold_in(own, 1), rows)]
    rotation = jax.random.randint(jax.random.fold_in(own, 2), (rows, 1), 0, top)
    return jnp.take_along_axis(listing, (jnp.arange(top)[None, :] + rotation) % top, axis=1)


def shares(count, total, reach, lean, full):
    loads = [(1 << 20) // math.isqrt(grade ** lean) + 1 for grade in range(1, count + 1)]
    largest = reach if full else min(reach, max(-(-total // count), total * loads[0] // sum(loads)))
    least = 1 if total - largest >= count - 1 else 0
    counts, rest = [largest] + [least] * (count - 1), total - largest - least * (count - 1)
    while rest > 0:
        candidates = [i for i in range(1, count) if counts[i] < largest] or [i for i in range(1, count) if counts[i] < reach]
        pool, budget = sum([loads[i] for i in candidates]), rest
        for i in candidates:
            addition = min(reach - counts[i], max(1, budget * loads[i] // pool), rest)
            counts[i] = counts[i] + addition
            rest = rest - addition
    return np.array(counts)


def scatter_about(own_key, extent, scale, reach, cuts=(), held_as=jnp.bfloat16):
    array = jax.random.normal(own_key, extent, jnp.float32) * scale
    if len(cuts) > 0:
        array = levels(own_key, extent, cuts, -0.22, 0.18) * array
    return jnp.clip(array, min=-reach, max=reach).astype(held_as)


def setup_inputs(seed: int = 0) -> dict:
    splits = jax.random.split(jax.random.key(seed), 18)
    tokens = scatter_about(splits[0], (SEQUENCE_TOTAL, D), 1.0, 6.0, ((0, 16),))
    lengths = with_ends(jax.random.randint(splits[1], (SEQUENCE_TOTAL,), CACHE_POSITIONS // 8, CACHE_POSITIONS + 1), jax.random.fold_in(splits[1], 1), CACHE_POSITIONS // 8, CACHE_POSITIONS).astype(jnp.int32)
    key_cache = draw_key_cache(jax.random.fold_in(splits[17], 71), 0)
    value_cache = scatter_about(splits[3], (SEQUENCE_TOTAL, CACHE_POSITIONS, KV_HEADS * HD), 1.0, 6.0, ((0, 16), (2, 2)))
    gate_cache = draw_gate_cache(jax.random.fold_in(splits[17], 71), 0)
    mix_gain = jnp.clip(1.0 + 0.18 * jax.random.normal(splits[5], (D,), jnp.float32), 0.1, 1.9)
    query_weight = scatter_about(splits[6], (D, HEADS * HD), D ** -0.5, 0.125, ((1, 2),))
    key_weight = scatter_about(splits[7], (D, KV_HEADS * HD), D ** -0.5, 0.125, ((1, 2),))
    value_weight = scatter_about(splits[8], (D, KV_HEADS * HD), D ** -0.5, 0.125, ((1, 2),))
    forget_weight = scatter_about(splits[9], (D, HEADS), D ** -0.5, 0.125, ((1, 2),))
    out_weight = scatter_about(splits[10], (HEADS * HD, D), (HEADS * HD) ** -0.5, 0.1875, ((0, 2),))
    expert_gain = jnp.clip(1.0 + 0.18 * jax.random.normal(splits[11], (D,), jnp.float32), 0.1, 1.9)
    routes_keys = jax.random.split(jax.random.fold_in(splits[12], 1), SEQUENCE_TOTAL // SEQ_DEV)
    routes_turns = jax.random.permutation(jax.random.fold_in(splits[12], 3), SEQUENCE_TOTAL // SEQ_DEV)
    routes = jax.vmap(lambda own, number: deal_out(jax.random.fold_in(splits[12], 2), own, number, SEQ_DEV, EXPERTS, TOP, CAP, 2))(routes_keys, routes_turns).reshape((SEQUENCE_TOTAL, TOP))
    route_weights = jnp.clip(0.2 + 0.8 * jax.random.uniform(splits[13], (SEQUENCE_TOTAL, TOP), jnp.float32) ** levels(splits[13], (SEQUENCE_TOTAL, TOP), ((0, 16),), -0.2, 0.2), 0.2, 1.0)
    expert_gate = scatter_about(splits[14], (D, EXPERTS * FF), D ** -0.5, 0.125, ((1, 32),))
    expert_up = scatter_about(splits[15], (D, EXPERTS * FF), D ** -0.5, 0.125, ((1, 32),))
    expert_down = scatter_about(splits[16], (EXPERTS * FF, D), FF ** -0.5, 0.0625, ((0, 32),))
    return dict(tokens=tokens, lengths=lengths, key_cache=key_cache, value_cache=value_cache, gate_cache=gate_cache, mix_gain=mix_gain, query_weight=query_weight, key_weight=key_weight, value_weight=value_weight, forget_weight=forget_weight, out_weight=out_weight, expert_gain=expert_gain, routes=routes, route_weights=route_weights, expert_gate=expert_gate, expert_up=expert_up, expert_down=expert_down)


eps = 1e-06

def normed(values, gain):
    floats = values.astype(jnp.float32)
    return floats * lax.rsqrt(lax.optimization_barrier(jnp.mean(floats * floats, axis=-1, keepdims=True)) + eps) * gain

def attend(pack):
    queries, key_new, value_new, log_gate, key_rows, value_rows, cumulative, length = pack
    seq_count, head_count, head_size = queries.shape
    kv_count = key_new.shape[1]
    group_size = head_count // kv_count
    cache_locations = key_rows.shape[1]
    factor = head_size ** (-0.5)
    grouped = queries.reshape(seq_count, kv_count, group_size, head_size).astype(jnp.float32)
    key_split = key_rows.reshape(seq_count, cache_locations, kv_count, head_size).astype(jnp.float32)
    value_split = value_rows.reshape(seq_count, cache_locations, kv_count, head_size).astype(jnp.float32)
    scores = jnp.einsum('skgd,spkd->skgp', grouped, key_split).reshape(seq_count, head_count, cache_locations) * factor
    positions = jnp.arange(cache_locations, dtype=jnp.int32)
    latest = lax.optimization_barrier(jnp.sum(jnp.where(positions[None, None, :] == (length - 1)[:, None, None], cumulative, 0.0), axis=-1))
    scores = scores + (latest + log_gate)[..., None] - cumulative
    valid = positions[None, None, :] < length[:, None, None]
    scores = jnp.where(valid, scores, -jnp.inf)
    own_score = jnp.einsum('skgd,skd->skg', grouped, key_new.astype(jnp.float32)).reshape(seq_count, head_count) * factor
    highest = jnp.maximum(lax.optimization_barrier(jnp.max(scores, axis=-1)), own_score)
    raised = jnp.exp(scores - highest[..., None])
    own_raised = jnp.exp(own_score - highest)
    denominator = lax.optimization_barrier(jnp.sum(raised, axis=-1)) + own_raised
    weights = (raised / denominator[..., None]).astype(jnp.bfloat16)
    own_weight = (own_raised / denominator).astype(jnp.bfloat16)
    mixed = jnp.einsum('skgp,spkd->skgd', weights.reshape(seq_count, kv_count, group_size, cache_locations).astype(jnp.float32), value_split)
    mixed = mixed + own_weight.reshape(seq_count, kv_count, group_size)[..., None].astype(jnp.float32) * value_new.astype(jnp.float32)[:, :, None, :]
    return mixed.reshape(seq_count, head_count * head_size).astype(jnp.bfloat16)

def reference(tokens, lengths, key_cache, value_cache, gate_cache, mix_gain, query_weight, key_weight, value_weight, forget_weight, out_weight, expert_gain, routes, route_weights, expert_gate, expert_up, expert_down):
    normal_in = normed(tokens, mix_gain).astype(jnp.bfloat16)
    queries = jnp.dot(normal_in, query_weight, preferred_element_type=jnp.float32).astype(jnp.bfloat16).reshape(N_EP, SEQ_DEV, HEADS, HD)
    key_new = jnp.dot(normal_in, key_weight, preferred_element_type=jnp.float32).astype(jnp.bfloat16).reshape(N_EP, SEQ_DEV, KV_HEADS, HD)
    value_new = jnp.dot(normal_in, value_weight, preferred_element_type=jnp.float32).astype(jnp.bfloat16).reshape(N_EP, SEQ_DEV, KV_HEADS, HD)
    log_gate = jax.nn.log_sigmoid(jnp.dot(normal_in, forget_weight, preferred_element_type=jnp.float32)).reshape(N_EP, SEQ_DEV, HEADS)
    mixed = lax.map(attend, (queries, key_new, value_new, log_gate, key_cache.reshape(N_EP, SEQ_DEV, CACHE_POSITIONS, KV_HEADS * HD), value_cache.reshape(N_EP, SEQ_DEV, CACHE_POSITIONS, KV_HEADS * HD), gate_cache.reshape(N_EP, SEQ_DEV, HEADS, CACHE_POSITIONS), lengths.reshape(N_EP, SEQ_DEV)))
    mixed = mixed.reshape(SEQUENCE_TOTAL, HEADS * HD)
    split = HEADS * HD // N_TP
    summed = tokens.astype(jnp.float32)
    for group_index in range(N_TP):
        product = jnp.dot(mixed[:, group_index * split:(group_index + 1) * split], out_weight[group_index * split:(group_index + 1) * split], preferred_element_type=jnp.float32)
        summed = summed + lax.optimization_barrier(product.astype(jnp.bfloat16)).astype(jnp.float32)
    residual = summed.astype(jnp.bfloat16)
    expert_in = normed(residual, expert_gain).astype(jnp.bfloat16)
    flat_routes = routes.reshape(N_EP, SEQ_DEV * TOP)
    one_hot = (flat_routes[..., None] == jnp.arange(EXPERTS, dtype=jnp.int32)).astype(jnp.int32)
    slot_index = lax.optimization_barrier(jnp.sum((jnp.cumsum(one_hot, axis=1) - 1) * one_hot, axis=-1))
    repeated = jnp.repeat(expert_in.reshape(N_EP, SEQ_DEV, D), TOP, axis=1).astype(jnp.float32)
    pieces = N_EP // EXPERTS
    quarter = FF // (pieces * N_TP)

    def one_expert(expert):
        chosen = (flat_routes == expert)[:, None, :] & (slot_index[:, None, :] == jnp.arange(CAP, dtype=jnp.int32)[None, :, None])
        rows_in = jnp.einsum('ncr,nrd->ncd', chosen.astype(jnp.float32), repeated).astype(jnp.bfloat16).reshape(N_EP * CAP, D)
        w_gate = lax.dynamic_slice_in_dim(expert_gate, expert * FF, FF, 1)
        w_up = lax.dynamic_slice_in_dim(expert_up, expert * FF, FF, 1)
        w_down = lax.dynamic_slice_in_dim(expert_down, expert * FF, FF, 0)
        gate_out = jnp.dot(rows_in, w_gate, preferred_element_type=jnp.float32)
        up_out = jnp.dot(rows_in, w_up, preferred_element_type=jnp.float32)
        hidden = (jax.nn.silu(gate_out) * up_out).astype(jnp.bfloat16)
        halves = jnp.einsum('rbtf,btfd->rbtd', hidden.reshape(N_EP * CAP, pieces, N_TP, quarter).astype(jnp.float32), w_down.reshape(pieces, N_TP, quarter, D).astype(jnp.float32))
        halves = lax.optimization_barrier(halves.astype(jnp.bfloat16)).astype(jnp.float32)
        blocks = lax.optimization_barrier(lax.optimization_barrier(jnp.sum(halves, axis=2)).astype(jnp.bfloat16)).astype(jnp.float32)
        return lax.optimization_barrier(jnp.sum(blocks, axis=1))
    results = lax.map(one_expert, jnp.arange(EXPERTS, dtype=jnp.int32))
    row_index = flat_routes * (N_EP * CAP) + jnp.arange(N_EP, dtype=jnp.int32)[:, None] * CAP + slot_index
    picked = jnp.take(results.reshape(EXPERTS * N_EP * CAP, D), row_index.reshape(-1).astype(jnp.int32), axis=0).reshape(SEQUENCE_TOTAL, TOP, D)
    mixture = lax.optimization_barrier(jnp.sum(picked * route_weights[..., None], axis=1))
    return (residual.astype(jnp.float32) + mixture).astype(jnp.bfloat16)
```

```python
import functools

import jax
import jax.numpy as jnp
from jax import lax
from jax.experimental import pallas as pl
from jax.experimental.pallas import tpu as pltpu
from jax.sharding import PartitionSpec as P

HD = 64
EXPERTS = 8
CAP = 12
LANES = 128
GROUP = 8
STEP = 128

eps = 1e-06
f32 = jnp.float32
bf16 = jnp.bfloat16
VMEM_SPEC = pl.BlockSpec(memory_space=pltpu.VMEM)
HBM_SPEC = pl.BlockSpec(memory_space=pltpu.HBM)
NT = (((1,), (1,)), ((), ()))
TN = (((0,), (0,)), ((), ()))


def in_hbm(array):
    return pltpu.with_memory_space_constraint(array, pltpu.HBM)


def in_vmem(array):
    return pltpu.with_memory_space_constraint(array, pltpu.VMEM)


def iota(shape, dim):
    return lax.broadcasted_iota(jnp.int32, shape, dim)


def quotient(values, divisor):
    return jnp.floor((values.astype(f32) + 0.5) * (1.0 / divisor))


def normed(values, gain):
    floats = values.astype(f32)
    return floats * lax.rsqrt(jnp.mean(floats * floats, axis=-1, keepdims=True) + eps) * gain


def slot_matrix(routes, rows, pieces):
    count = routes.shape[1]
    first, second = routes[0:1, :], routes[1:2, :]
    expert = iota((EXPERTS, count), 0)
    named = ((first == expert) | (second == expert)).astype(f32).astype(bf16)
    earlier = (iota((count, count), 0) < iota((count, count), 1)).astype(f32).astype(bf16)
    slot = jnp.dot(named, earlier, preferred_element_type=f32) + (expert * CAP).astype(f32)
    place0 = jnp.sum(jnp.where(first == expert, slot, 0.0), axis=0, keepdims=True)
    place1 = jnp.sum(jnp.where(second == expert, slot, 0.0), axis=0, keepdims=True)
    unused = jnp.full((1, 2 * count), -1.0, f32)
    lower = jnp.concatenate([place0, place1, unused], axis=1)
    upper = jnp.concatenate([unused, place0, place1], axis=1)
    row = iota((rows, 4 * count), 0)
    block = quotient(row, 2 * CAP)
    within = row.astype(f32) - block * (2 * CAP)
    half = within >= CAP
    wanted = quotient(block, pieces) * CAP + jnp.where(half, within - CAP, within)
    hit = jnp.where(half, (wanted == upper).astype(f32), (wanted == lower).astype(f32))
    return hit.astype(bf16)


def attention_kernel(
    pieces,
    lengths_in,
    tokens,
    gain,
    forget,
    routes,
    wq,
    wk,
    wv,
    wo,
    keys,
    values,
    gates,
    partial_out,
    slots,
    lengths_s,
    tokens_v,
    gain_v,
    forget_v,
    routes_v,
    wq_v,
    wk_v,
    wv_v,
    wo_v,
    keys_v,
    values_v,
    gates_v,
    query_v,
    key_new_v,
    value_new_v,
    log_gate_v,
    mixed_v,
    small_sem,
    weight_sem,
    gate_sem,
    key_sem,
    value_sem,
):
    seq_count, positions, _ = keys.shape
    heads = gates.shape[1]
    pairs = heads // 2
    groups = seq_count // GROUP

    lengths = lengths_s
    small = [
        pltpu.make_async_copy(src, dst, small_sem.at[i])
        for i, (src, dst) in enumerate(
            (
                (lengths_in, lengths_s),
                (routes, routes_v),
                (tokens, tokens_v),
                (gain, gain_v),
                (forget, forget_v),
            )
        )
    ]
    copies = [
        pltpu.make_async_copy(src, dst, weight_sem.at[i])
        for i, (src, dst) in enumerate(((wq, wq_v), (wk, wk_v), (wv, wv_v), (wo, wo_v)))
    ]

    def used(s):
        return pl.multiple_of((lengths[s] + STEP - 1) // STEP * STEP, STEP)

    def key_copy(s):
        window = pl.ds(0, used(s))
        return pltpu.make_async_copy(keys.at[s, window], keys_v.at[s, window], key_sem.at[s])

    def value_copy(s):
        window = pl.ds(0, used(s))
        return pltpu.make_async_copy(values.at[s, window], values_v.at[s, window], value_sem.at[s])

    def gate_copy(g):
        window = pl.ds(g * GROUP, GROUP)
        return pltpu.make_async_copy(gates.at[window], gates_v.at[window], gate_sem.at[g])

    for c in small + copies[:3]:
        c.start()

    def start_keys(g):
        gate_copy(g).start()
        for j in range(GROUP):
            key_copy(g * GROUP + j).start()

    def start_values(g):
        for j in range(GROUP):
            value_copy(g * GROUP + j).start()

    small[0].wait()
    start_keys(0)

    def clear(s, _):
        values_v[s] = jnp.zeros(values_v.shape[1:], bf16)
        return 0

    lax.fori_loop(0, seq_count, clear, 0)
    start_values(0)

    def start_rest(g, _):
        start_keys(g)
        start_values(g)
        return 0

    lax.fori_loop(1, groups, start_rest, 0)
    copies[3].start()

    for c in small[1:]:
        c.wait()
    slots[...] = slot_matrix(routes_v[...], slots.shape[0], pieces)

    normal_in = normed(tokens_v[...], gain_v[...]).astype(bf16)
    gate_in = lax.dot_general(forget_v[...], normal_in, NT, preferred_element_type=f32)
    log_gate_v[:, :seq_count] = jnp.minimum(gate_in, 0.0) - jnp.log1p(jnp.exp(-jnp.abs(gate_in)))
    low = iota((seq_count, LANES), 1) < HD
    for c in copies[:3]:
        c.wait()
    query = jnp.dot(normal_in, wq_v[...], preferred_element_type=f32).astype(bf16).astype(f32)
    query = query * (HD**-0.5)
    key_new_v[...] = (
        jnp.dot(normal_in, wk_v[...], preferred_element_type=f32).astype(bf16).astype(f32)
    )
    value_new_v[...] = (
        jnp.dot(normal_in, wv_v[...], preferred_element_type=f32).astype(bf16).astype(f32)
    )
    for j in range(pairs):
        val = query[:, j * LANES : (j + 1) * LANES]
        turned = pltpu.roll(val, HD, 1)
        if j < pairs // 2:
            one, two = jnp.where(low, val, 0.0), jnp.where(low, turned, 0.0)
        else:
            one, two = jnp.where(low, 0.0, turned), jnp.where(low, 0.0, val)
        query_v[:, 2 * j, :] = one
        query_v[:, 2 * j + 1, :] = two

    lane = iota((heads, LANES), 1)
    position = iota((heads, positions), 1)

    def group_step(g, _):
        gate_copy(g).wait()
        scored = []
        for j in range(GROUP):
            s = g * GROUP + j
            key_copy(s).wait()
        for j in range(GROUP):
            s = g * GROUP + j
            length = lengths[s]
            query_s = query_v[s]
            score = lax.dot_general(
                query_s.astype(bf16), keys_v[s], NT, preferred_element_type=f32
            )
            last = length - 1
            start = pl.multiple_of(last // LANES * LANES, LANES)
            near = gates_v[s, :, pl.ds(start, LANES)]
            picked = jnp.where(lane == last - start, near, 0.0) + jnp.where(
                lane == s, log_gate_v[...], 0.0
            )
            offset = jnp.sum(picked, axis=1, keepdims=True)
            own = jnp.sum(query_s * key_new_v[pl.ds(s, 1), :], axis=1, keepdims=True)
            score = jnp.where(position < length, score + offset - gates_v[s], -jnp.inf)
            highest = jnp.maximum(jnp.max(score, axis=1, keepdims=True), own)
            raised = jnp.exp(score - highest)
            own_raised = jnp.exp(own - highest)
            total = jnp.sum(raised, axis=1, keepdims=True) + own_raised
            scored.append((raised.astype(bf16), own_raised, total))
        for j in range(GROUP):
            s = g * GROUP + j
            value_copy(s).wait()
        for j in range(GROUP):
            s = g * GROUP + j
            raised, own_raised, total = scored[j]
            product = jnp.dot(raised, values_v[s], preferred_element_type=f32)
            product = product + own_raised * value_new_v[pl.ds(s, 1), :]
            mixed_v[s] = product / total
        return 0

    lax.fori_loop(0, groups, group_step, 0)

    parts = []
    for j in range(pairs):
        one, two = mixed_v[:, 2 * j, :], mixed_v[:, 2 * j + 1, :]
        if j < pairs // 2:
            parts.append(jnp.where(low, one, pltpu.roll(two, HD, 1)))
        else:
            parts.append(jnp.where(low, pltpu.roll(one, HD, 1), two))
    mixed = jnp.concatenate(parts, axis=1).astype(bf16)
    copies[3].wait()
    partial_out[...] = jnp.dot(mixed, wo_v[...], preferred_element_type=f32).astype(bf16)


def dispatch_kernel(tokens, own, other, gain, slots, outgoing, own_half, normal_v, full_v):
    columns = own_half.shape[1]
    quarter = columns // 2
    residual = tokens[...].astype(f32) + own[...].astype(f32) + other[...].astype(f32)
    residual = residual.astype(bf16)
    full_v[...] = residual
    normal_v[...] = normed(residual, gain[...]).astype(bf16)
    start = pl.multiple_of(lax.axis_index("tp") * columns, columns)
    own_half[...] = full_v[:, pl.ds(start, columns)]
    first = normal_v[:, pl.ds(start, quarter)]
    second = normal_v[:, pl.ds(pl.multiple_of(start + quarter, quarter), quarter)]
    stacked = jnp.concatenate([first, first, second, second], axis=0)
    outgoing[...] = jnp.dot(slots[...], stacked, preferred_element_type=f32).astype(bf16)


def gather_matrix(rows_in, rows_out, half, turned):
    shape = (rows_in, rows_out) if turned else (rows_out, rows_in)
    dim = 1 if turned else 0
    row = iota(shape, dim)
    source = quotient(row, CAP)
    target = source * (2 * CAP) + half * CAP + (row.astype(f32) - source * CAP)
    return (target == iota(shape, 1 - dim).astype(f32)).astype(f32).astype(bf16)


def expert_kernel(
    parts,
    mine,
    others,
    w_gate,
    w_up,
    w_down,
    out_mine,
    out_others,
    rows_v,
    hidden_v,
    down_v,
    down_sem,
):
    width, units = w_gate.shape
    block = units // parts
    columns = width // 2
    quarter = columns // 2
    me = lax.axis_index("tp")

    def down_start(q):
        return pl.multiple_of(jnp.where(q < 2, 1 - me, me) * columns + (q % 2) * quarter, quarter)

    def down_copy(q):
        window = pl.ds(down_start(q), quarter)
        return pltpu.make_async_copy(w_down.at[:, window], down_v.at[q], down_sem.at[q])

    for q in range(4):
        down_copy(q).start()

    rows_in = mine.shape[0]
    rows_out = rows_in // 2
    span = min(rows_in, 16 * 2 * CAP)
    span_out = span // 2
    for half in range(2):
        matrix = gather_matrix(span, span_out, half, False)
        for piece in range(rows_in // span):
            taken = pl.ds(piece * span, span)
            given = pl.ds(piece * span_out, span_out)
            for source, side in ((mine, me), (others, 1 - me)):
                start = pl.multiple_of(side * columns + half * quarter, quarter)
                rows_v[given, pl.ds(start, quarter)] = jnp.dot(
                    matrix, source[taken, :], preferred_element_type=f32
                ).astype(bf16)

    for j in range(parts):
        window = slice(j * block, (j + 1) * block)
        gate_out = jnp.dot(rows_v[...], w_gate[:, window], preferred_element_type=f32)
        up_out = jnp.dot(rows_v[...], w_up[:, window], preferred_element_type=f32)
        hidden = gate_out * jax.nn.sigmoid(gate_out) * up_out
        hidden_v[:, j * block : (j + 1) * block] = hidden.astype(bf16)

    spread = [gather_matrix(span, span_out, half, True) for half in range(2)]
    for side, target in ((0, out_others), (1, out_mine)):
        results = []
        for half in range(2):
            q = 2 * side + half
            down_copy(q).wait()
            results.append(
                jnp.dot(hidden_v[...], down_v[q], preferred_element_type=f32).astype(bf16)
            )
        for piece in range(rows_in // span):
            taken = slice(piece * span_out, (piece + 1) * span_out)
            target[pl.ds(piece * span, span), :] = (
                jnp.dot(spread[0], results[0][taken], preferred_element_type=f32)
                + jnp.dot(spread[1], results[1][taken], preferred_element_type=f32)
            ).astype(bf16)


def combine_kernel(returned, slots, own_half, route_weights, out):
    seq_count = own_half.shape[0]
    quarter = returned.shape[1]
    picked = lax.dot_general(slots[...], returned[...], TN, preferred_element_type=f32)
    square = iota((seq_count, seq_count), 0) == iota((seq_count, seq_count), 1)
    weights = [
        jnp.sum(jnp.where(square, route_weights[k : k + 1, :], 0.0), axis=1, keepdims=True)
        for k in range(2)
    ]
    for half in range(2):
        base = half * 2 * seq_count
        mixture = picked[base : base + seq_count] * weights[0]
        mixture = mixture + picked[base + seq_count : base + 2 * seq_count] * weights[1]
        span = slice(half * quarter, (half + 1) * quarter)
        out[:, span] = (own_half[:, span].astype(f32) + mixture).astype(bf16)


def on_device(
    tokens,
    lengths,
    key_cache,
    value_cache,
    gate_cache,
    mix_gain,
    query_weight,
    key_weight,
    value_weight,
    forget_weight,
    out_weight,
    expert_gain,
    routes,
    route_weights,
    expert_gate,
    expert_up,
    expert_down,
):
    seq_count, width = tokens.shape
    positions = key_cache.shape[1]
    heads = gate_cache.shape[1]
    chips = lax.axis_size("ep")
    pieces = chips // EXPERTS
    rows = chips * 2 * CAP
    columns = width // 2
    quarter = columns // 2
    groups = seq_count // GROUP
    swap = [(0, 1), (1, 0)]
    dma = pltpu.SemaphoreType.DMA

    partial_out, slots = pl.pallas_call(
        functools.partial(attention_kernel, pieces),
        name="attention",
        out_shape=(
            jax.ShapeDtypeStruct((seq_count, width), bf16),
            jax.ShapeDtypeStruct((rows, 4 * seq_count), bf16),
        ),
        in_specs=[HBM_SPEC] * 12,
        out_specs=(VMEM_SPEC, VMEM_SPEC),
        scratch_shapes=[
            pltpu.SMEM((seq_count,), jnp.int32),
            pltpu.VMEM((seq_count, width), bf16),
            pltpu.VMEM((1, width), f32),
            pltpu.VMEM((heads, width), bf16),
            pltpu.VMEM((2, seq_count), jnp.int32),
            pltpu.VMEM(query_weight.shape, bf16),
            pltpu.VMEM(key_weight.shape, bf16),
            pltpu.VMEM(value_weight.shape, bf16),
            pltpu.VMEM(out_weight.shape, bf16),
            pltpu.VMEM(key_cache.shape, bf16),
            pltpu.VMEM(value_cache.shape, bf16),
            pltpu.VMEM(gate_cache.shape, f32),
            pltpu.VMEM((seq_count, heads, LANES), f32),
            pltpu.VMEM((seq_count, LANES), f32),
            pltpu.VMEM((seq_count, LANES), f32),
            pltpu.VMEM((heads, LANES), f32),
            pltpu.VMEM((seq_count, heads, LANES), f32),
            dma((5,)),
            dma((4,)),
            dma((groups,)),
            dma((seq_count,)),
            dma((seq_count,)),
        ],
        compiler_params=pltpu.CompilerParams(vmem_limit_bytes=25 << 20),
    )(
        *map(
            in_hbm,
            (
                lengths,
                tokens,
                mix_gain.reshape(1, width),
                forget_weight.T,
                routes.T,
                query_weight,
                key_weight,
                value_weight,
                out_weight,
                key_cache,
                value_cache,
                gate_cache,
            ),
        ),
    )
    other_out = lax.ppermute(partial_out, "tp", swap)

    outgoing, own_half = pl.pallas_call(
        dispatch_kernel,
        name="dispatch",
        out_shape=(
            jax.ShapeDtypeStruct((rows, quarter), bf16),
            jax.ShapeDtypeStruct((seq_count, columns), bf16),
        ),
        in_specs=[VMEM_SPEC] * 5,
        out_specs=(VMEM_SPEC, VMEM_SPEC),
        scratch_shapes=[
            pltpu.VMEM((seq_count, width), bf16),
            pltpu.VMEM((seq_count, width), bf16),
        ],
        compiler_params=pltpu.CompilerParams(vmem_limit_bytes=8 << 20),
    )(tokens, partial_out, other_out, expert_gain.reshape(1, width), slots)

    received = lax.all_to_all(
        outgoing.reshape(chips, 2 * CAP, quarter), "ep", split_axis=0, concat_axis=0, tiled=True
    )
    others = lax.ppermute(received, "tp", swap)

    units = expert_gate.shape[1]
    parts = max(1, units // 512)
    in_rows = chips * CAP
    back_mine, back_others = pl.pallas_call(
        functools.partial(expert_kernel, parts),
        name="experts",
        out_shape=(jax.ShapeDtypeStruct((rows, quarter), bf16),) * 2,
        in_specs=[VMEM_SPEC] * 4 + [HBM_SPEC],
        out_specs=(VMEM_SPEC, VMEM_SPEC),
        scratch_shapes=[
            pltpu.VMEM((in_rows, width), bf16),
            pltpu.VMEM((in_rows, units), bf16),
            pltpu.VMEM((4, units, quarter), bf16),
            dma((4,)),
        ],
        compiler_params=pltpu.CompilerParams(vmem_limit_bytes=20 << 20),
    )(
        received.reshape(rows, quarter),
        others.reshape(rows, quarter),
        in_vmem(expert_gate),
        in_vmem(expert_up),
        in_hbm(expert_down),
    )
    from_other = lax.ppermute(back_others, "tp", swap)
    share = (back_mine.astype(f32) + from_other.astype(f32)).astype(bf16)
    returned = lax.all_to_all(
        share.reshape(chips, 2 * CAP, quarter), "ep", split_axis=0, concat_axis=0, tiled=True
    )
    half = pl.pallas_call(
        combine_kernel,
        name="combine",
        out_shape=jax.ShapeDtypeStruct((seq_count, columns), bf16),
        in_specs=[VMEM_SPEC] * 4,
        out_specs=VMEM_SPEC,
        compiler_params=pltpu.CompilerParams(vmem_limit_bytes=8 << 20),
    )(returned.reshape(rows, quarter), slots, own_half, route_weights.T)
    return lax.all_gather(half, "tp", axis=1, tiled=True)


def solution(mesh):
    return jax.shard_map(
        on_device,
        mesh=mesh,
        in_specs=(
            P("ep", None),
            P("ep"),
            P("ep", None, "tp"),
            P("ep", None, "tp"),
            P("ep", "tp", None),
            P(),
            P(None, "tp"),
            P(None, "tp"),
            P(None, "tp"),
            P(None, "tp"),
            P("tp", None),
            P(),
            P("ep", None),
            P("ep", None),
            P(None, ("ep", "tp")),
            P(None, ("ep", "tp")),
            P(("ep", "tp"), None),
        ),
        out_specs=P("ep", None),
        check_vma=False,
    )
```

```python
import functools

import jax
import jax.numpy as jnp
from jax import lax
from jax.experimental import pallas as pl
from jax.experimental.pallas import tpu as pltpu
from jax.sharding import PartitionSpec as P

HD = 64
EXPERTS = 8
CAP = 12
LANES = 128
GROUP = 8
STEP = 128
COVER = 10**12

eps = 1e-06
f32 = jnp.float32
bf16 = jnp.bfloat16
VMEM_SPEC = pl.BlockSpec(memory_space=pltpu.VMEM)
HBM_SPEC = pl.BlockSpec(memory_space=pltpu.HBM)
NT = (((1,), (1,)), ((), ()))
TN = (((0,), (0,)), ((), ()))


def in_hbm(array):
    return pltpu.with_memory_space_constraint(array, pltpu.HBM)


def in_vmem(array):
    return pltpu.with_memory_space_constraint(array, pltpu.VMEM)


def iota(shape, dim):
    return lax.broadcasted_iota(jnp.int32, shape, dim)


def quotient(values, divisor):
    return jnp.floor((values.astype(f32) + 0.5) * (1.0 / divisor))


def normed(values, gain):
    floats = values.astype(f32)
    return floats * lax.rsqrt(jnp.mean(floats * floats, axis=-1, keepdims=True) + eps) * gain


def slot_matrix(routes, rows, pieces):
    count = routes.shape[1]
    first, second = routes[0:1, :], routes[1:2, :]
    expert = iota((EXPERTS, count), 0)
    named = ((first == expert) | (second == expert)).astype(f32).astype(bf16)
    earlier = (iota((count, count), 0) < iota((count, count), 1)).astype(f32).astype(bf16)
    slot = jnp.dot(named, earlier, preferred_element_type=f32) + (expert * CAP).astype(f32)
    place0 = jnp.sum(jnp.where(first == expert, slot, 0.0), axis=0, keepdims=True)
    place1 = jnp.sum(jnp.where(second == expert, slot, 0.0), axis=0, keepdims=True)
    unused = jnp.full((1, 2 * count), -1.0, f32)
    lower = jnp.concatenate([place0, place1, unused], axis=1)
    upper = jnp.concatenate([unused, place0, place1], axis=1)
    row = iota((rows, 4 * count), 0)
    block = quotient(row, 2 * CAP)
    within = row.astype(f32) - block * (2 * CAP)
    half = within >= CAP
    wanted = quotient(block, pieces) * CAP + jnp.where(half, within - CAP, within)
    hit = jnp.where(half, (wanted == upper).astype(f32), (wanted == lower).astype(f32))
    return hit.astype(bf16)


def sort_table(row):
    count = row.shape[1]
    lane, sub = iota((count, count), 1), iota((count, count), 0)
    column = jnp.sum(jnp.where(lane == sub, row, 0), axis=1, keepdims=True)
    before = (row > column) | ((row == column) & (lane < sub))
    rank = jnp.sum(before.astype(f32), axis=1, keepdims=True)
    lane, sub = iota((count, LANES), 1), iota((count, LANES), 0)
    hit = rank == lane.astype(f32)
    order = jnp.sum(jnp.where(hit, sub, 0), axis=0, keepdims=True)
    length = jnp.sum(jnp.where(hit, column, 0), axis=0, keepdims=True)
    return order, length


def attention_kernel(
    pieces,
    lengths,
    tokens,
    gain,
    second_gain,
    forget,
    routes,
    wq,
    wk,
    wv,
    wo,
    keys,
    values,
    gates,
    partial_out,
    slots,
    tokens_v,
    second_gain_v,
    lengths_v,
    table_v,
    table_s,
    gain_v,
    forget_v,
    routes_v,
    wq_v,
    wk_v,
    wv_v,
    wo_v,
    keys_v,
    values_v,
    gates_v,
    query_v,
    key_new_v,
    value_new_v,
    log_gate_v,
    mixed_v,
    small_sem,
    weight_sem,
    base_sem,
    key_sem,
    value_sem,
):
    seq_count, positions, _ = keys.shape
    heads = gates.shape[1]
    pairs = heads // 2
    groups = seq_count // GROUP

    small = [
        pltpu.make_async_copy(src, dst, small_sem.at[i])
        for i, (src, dst) in enumerate(
            (
                (lengths, lengths_v),
                (tokens, tokens_v),
                (gain, gain_v),
                (forget, forget_v),
                (routes, routes_v),
                (second_gain, second_gain_v),
            )
        )
    ]
    table_copy = pltpu.make_async_copy(table_v, table_s, small_sem.at[6])
    copies = [
        pltpu.make_async_copy(src, dst, weight_sem.at[i])
        for i, (src, dst) in enumerate(((wq, wq_v), (wk, wk_v), (wv, wv_v), (wo, wo_v)))
    ]

    every = pl.ds(0, seq_count)
    base = pl.ds(0, STEP)
    gate_copy = pltpu.make_async_copy(gates, gates_v, base_sem.at[0])
    key_base = pltpu.make_async_copy(keys.at[every, base], keys_v.at[every, base], base_sem.at[1])
    value_base = pltpu.make_async_copy(
        values.at[every, base], values_v.at[every, base], base_sem.at[2]
    )

    def chunks(g):
        return (table_s[1, g * GROUP] + STEP - 1) // STEP

    def group_copies(g):
        window = pl.ds(STEP, pl.multiple_of((chunks(g) - 1) * STEP, STEP))
        pairs_of = []
        for j in range(GROUP):
            s = table_s[0, g * GROUP + j]
            pairs_of.append(
                (
                    pltpu.make_async_copy(keys.at[s, window], keys_v.at[s, window], key_sem.at[s]),
                    pltpu.make_async_copy(
                        values.at[s, window], values_v.at[s, window], value_sem.at[s]
                    ),
                )
            )
        return pairs_of

    for c in small + copies[:3] + [gate_copy, key_base, value_base, copies[3]]:
        c.start()
    small[0].wait()
    order, length = sort_table(lengths_v[...])
    table_v[0:1, :] = order
    table_v[1:2, :] = length
    table_copy.start()
    table_copy.wait()

    def start_group(g, _):
        @pl.when(chunks(g) > 1)
        def _():
            copies_of = group_copies(g)
            for key_copy, _ in copies_of:
                key_copy.start()
            for _, value_copy in copies_of:
                value_copy.start()

        return 0

    lax.fori_loop(0, groups, start_group, 0)

    for c in small[1:]:
        c.wait()
    normal_in = normed(tokens_v[...], gain_v[...]).astype(bf16)
    gate_in = lax.dot_general(forget_v[...], normal_in, NT, preferred_element_type=f32)
    log_gate_v[:, :seq_count] = jnp.minimum(gate_in, 0.0) - jnp.log1p(jnp.exp(-jnp.abs(gate_in)))
    slots[...] = slot_matrix(routes_v[...], slots.shape[0], pieces)
    low = iota((seq_count, LANES), 1) < HD
    for c in copies[:3]:
        c.wait()
    query = jnp.dot(normal_in, wq_v[...], preferred_element_type=f32).astype(bf16).astype(f32)
    query = query * (HD**-0.5)
    key_new_v[...] = (
        jnp.dot(normal_in, wk_v[...], preferred_element_type=f32).astype(bf16).astype(f32)
    )
    value_new_v[...] = (
        jnp.dot(normal_in, wv_v[...], preferred_element_type=f32).astype(bf16).astype(f32)
    )
    for j in range(pairs):
        val = query[:, j * LANES : (j + 1) * LANES]
        turned = pltpu.roll(val, HD, 1)
        if j < pairs // 2:
            one, two = jnp.where(low, val, 0.0), jnp.where(low, turned, 0.0)
        else:
            one, two = jnp.where(low, 0.0, turned), jnp.where(low, 0.0, val)
        query_v[:, 2 * j, :] = one
        query_v[:, 2 * j + 1, :] = two

    lane = iota((heads, LANES), 1)

    def attend(g, reach):
        position = iota((heads, reach), 1)
        scored = []
        for j in range(GROUP):
            i = g * GROUP + j
            s, length = table_s[0, i], table_s[1, i]
            query_s = query_v[s]
            score = lax.dot_general(
                query_s.astype(bf16), keys_v[s, :reach], NT, preferred_element_type=f32
            )
            last = length - 1
            start = pl.multiple_of(last // LANES * LANES, LANES)
            near = gates_v[s, :, pl.ds(start, LANES)]
            picked = jnp.where(lane == last - start, near, 0.0) + jnp.where(
                lane == s, log_gate_v[...], 0.0
            )
            offset = jnp.sum(picked, axis=1, keepdims=True)
            own = jnp.sum(query_s * key_new_v[pl.ds(s, 1), :], axis=1, keepdims=True)
            score = jnp.where(position < length, score + offset - gates_v[s, :, :reach], -jnp.inf)
            highest = jnp.maximum(jnp.max(score, axis=1, keepdims=True), own)
            raised = jnp.exp(score - highest)
            own_raised = jnp.exp(own - highest)
            total = jnp.sum(raised, axis=1, keepdims=True) + own_raised
            scored.append((s, raised.astype(bf16), own_raised, total))
        for j in range(GROUP):
            s, raised, own_raised, total = scored[j]
            product = jnp.dot(raised, values_v[s, :reach], preferred_element_type=f32)
            product = product + own_raised * value_new_v[pl.ds(s, 1), :]
            mixed_v[s] = product / total

    for c in (gate_copy, key_base, value_base):
        c.wait()

    def group_step(g, _):
        count = chunks(g)

        @pl.when(count > 1)
        def _():
            for key_copy, value_copy in group_copies(g):
                key_copy.wait()
                value_copy.wait()

        for n in range(1, positions // STEP + 1):
            pl.when(count == n)(functools.partial(attend, g, n * STEP))
        return 0

    lax.fori_loop(0, groups, group_step, 0)

    parts = []
    for j in range(pairs):
        one, two = mixed_v[:, 2 * j, :], mixed_v[:, 2 * j + 1, :]
        if j < pairs // 2:
            parts.append(jnp.where(low, one, pltpu.roll(two, HD, 1)))
        else:
            parts.append(jnp.where(low, pltpu.roll(one, HD, 1), two))
    mixed = jnp.concatenate(parts, axis=1).astype(bf16)
    copies[3].wait()
    partial_out[...] = jnp.dot(mixed, wo_v[...], preferred_element_type=f32).astype(bf16)


def dispatch_kernel(tokens, own, other, gain, slots, outgoing, own_half, normal_v, full_v):
    columns = own_half.shape[1]
    quarter = columns // 2
    residual = tokens[...].astype(f32) + own[...].astype(f32) + other[...].astype(f32)
    residual = residual.astype(bf16)
    full_v[...] = residual
    normal_v[...] = normed(residual, gain[...]).astype(bf16)
    start = pl.multiple_of(lax.axis_index("tp") * columns, columns)
    own_half[...] = full_v[:, pl.ds(start, columns)]
    first = normal_v[:, pl.ds(start, quarter)]
    second = normal_v[:, pl.ds(pl.multiple_of(start + quarter, quarter), quarter)]
    stacked = jnp.concatenate([first, first, second, second], axis=0)
    outgoing[...] = jnp.dot(slots[...], stacked, preferred_element_type=f32).astype(bf16)


def gather_matrix(rows_in, rows_out, half, turned):
    shape = (rows_in, rows_out) if turned else (rows_out, rows_in)
    dim = 1 if turned else 0
    row = iota(shape, dim)
    source = quotient(row, CAP)
    target = source * (2 * CAP) + half * CAP + (row.astype(f32) - source * CAP)
    return (target == iota(shape, 1 - dim).astype(f32)).astype(f32).astype(bf16)


def unpack_rows(source, rows_v):
    quarter = source.shape[1]
    rows_in = source.shape[0]
    span = min(rows_in, 16 * 2 * CAP)
    for half in range(2):
        matrix = gather_matrix(span, span // 2, half, False)
        for piece in range(rows_in // span):
            rows_v[
                piece * (span // 2) : (piece + 1) * (span // 2),
                half * quarter : (half + 1) * quarter,
            ] = jnp.dot(
                matrix, source[piece * span : (piece + 1) * span, :], preferred_element_type=f32
            ).astype(bf16)


def down_rows(hidden, w_down, target, side, quarter):
    rows_in = target.shape[0]
    span = min(rows_in, 16 * 2 * CAP)
    results = []
    for half in range(2):
        start = pl.multiple_of(side * 2 * quarter + half * quarter, quarter)
        results.append(
            jnp.dot(
                hidden[...], w_down[:, pl.ds(start, quarter)], preferred_element_type=f32
            ).astype(bf16)
        )
    spread = [gather_matrix(span, span // 2, half, True) for half in range(2)]
    for piece in range(rows_in // span):
        taken = slice(piece * (span // 2), (piece + 1) * (span // 2))
        target[piece * span : (piece + 1) * span, :] = (
            jnp.dot(spread[0], results[0][taken], preferred_element_type=f32)
            + jnp.dot(spread[1], results[1][taken], preferred_element_type=f32)
        ).astype(bf16)


def first_kernel(parts, mine, w_gate, w_up, partial, rows_v):
    units = w_gate.shape[1]
    columns = rows_v.shape[1]
    block = units // parts
    rows = pl.ds(pl.multiple_of(lax.axis_index("tp") * columns, columns), columns)
    unpack_rows(mine, rows_v)
    for j in range(parts):
        window = slice(j * block, (j + 1) * block)
        for k, weight in enumerate((w_gate, w_up)):
            partial[k, :, window] = jnp.dot(
                rows_v[...], weight[rows, window], preferred_element_type=f32
            )


def second_kernel(
    parts, others, partial, w_gate, w_up, w_down, hidden_out, out_others, rows_v
):
    units = w_gate.shape[1]
    columns = rows_v.shape[1]
    block = units // parts
    side = 1 - lax.axis_index("tp")
    rows = pl.ds(pl.multiple_of(side * columns, columns), columns)
    unpack_rows(others, rows_v)
    for j in range(parts):
        window = slice(j * block, (j + 1) * block)
        gate_out, up_out = [
            partial[k, :, window]
            + jnp.dot(rows_v[...], weight[rows, window], preferred_element_type=f32)
            for k, weight in enumerate((w_gate, w_up))
        ]
        hidden = gate_out * jax.nn.sigmoid(gate_out) * up_out
        hidden_out[:, window] = hidden.astype(bf16)
    down_rows(hidden_out, w_down, out_others, side, others.shape[1])


def third_kernel(hidden, w_down, out_mine):
    down_rows(hidden, w_down, out_mine, lax.axis_index("tp"), out_mine.shape[1])


def combine_kernel(returned, slots, own_half, route_weights, out):
    seq_count = own_half.shape[0]
    quarter = returned.shape[1]
    picked = lax.dot_general(slots[...], returned[...], TN, preferred_element_type=f32)
    square = iota((seq_count, seq_count), 0) == iota((seq_count, seq_count), 1)
    weights = [
        jnp.sum(jnp.where(square, route_weights[k : k + 1, :], 0.0), axis=1, keepdims=True)
        for k in range(2)
    ]
    for half in range(2):
        base = half * 2 * seq_count
        mixture = picked[base : base + seq_count] * weights[0]
        mixture = mixture + picked[base + seq_count : base + 2 * seq_count] * weights[1]
        span = slice(half * quarter, (half + 1) * quarter)
        out[:, span] = (own_half[:, span].astype(f32) + mixture).astype(bf16)


def join_kernel(half, other, out, sem):
    columns = half.shape[1]
    me = lax.axis_index("tp")
    copies = [
        pltpu.make_async_copy(
            source,
            out.at[:, pl.ds(pl.multiple_of(side * columns, columns), columns)],
            sem.at[i],
        )
        for i, (source, side) in enumerate(((half, me), (other, 1 - me)))
    ]
    for c in copies:
        c.start()
    for c in copies:
        c.wait()


def on_device(
    tokens,
    lengths,
    key_cache,
    value_cache,
    gate_cache,
    mix_gain,
    query_weight,
    key_weight,
    value_weight,
    forget_weight,
    out_weight,
    expert_gain,
    routes,
    route_weights,
    expert_gate,
    expert_up,
    expert_down,
):
    seq_count, width = tokens.shape
    positions = key_cache.shape[1]
    heads = gate_cache.shape[1]
    chips = lax.axis_size("ep")
    pieces = chips // EXPERTS
    rows = chips * 2 * CAP
    columns = width // 2
    quarter = columns // 2
    swap = [(0, 1), (1, 0)]
    dma = pltpu.SemaphoreType.DMA

    partial_out, slots, tokens_out, gain_out = pl.pallas_call(
        functools.partial(attention_kernel, pieces),
        name="attention",
        out_shape=(
            pltpu.VMEM((seq_count, width), bf16),
            pltpu.VMEM((rows, 4 * seq_count), bf16),
            pltpu.VMEM((seq_count, width), bf16),
            pltpu.VMEM((1, width), f32),
        ),
        in_specs=[HBM_SPEC] * 13,
        out_specs=(VMEM_SPEC,) * 4,
        scratch_shapes=[
            pltpu.VMEM((1, seq_count), jnp.int32),
            pltpu.VMEM((2, LANES), jnp.int32),
            pltpu.SMEM((2, LANES), jnp.int32),
            pltpu.VMEM((1, width), f32),
            pltpu.VMEM((heads, width), bf16),
            pltpu.VMEM((2, seq_count), jnp.int32),
            pltpu.VMEM(query_weight.shape, bf16),
            pltpu.VMEM(key_weight.shape, bf16),
            pltpu.VMEM(value_weight.shape, bf16),
            pltpu.VMEM(out_weight.shape, bf16),
            pltpu.VMEM(key_cache.shape, bf16),
            pltpu.VMEM(value_cache.shape, bf16),
            pltpu.VMEM(gate_cache.shape, f32),
            pltpu.VMEM((seq_count, heads, LANES), f32),
            pltpu.VMEM((seq_count, LANES), f32),
            pltpu.VMEM((seq_count, LANES), f32),
            pltpu.VMEM((heads, LANES), f32),
            pltpu.VMEM((seq_count, heads, LANES), f32),
            dma((7,)),
            dma((4,)),
            dma((3,)),
            dma((seq_count,)),
            dma((seq_count,)),
        ],
        compiler_params=pltpu.CompilerParams(vmem_limit_bytes=59 << 20),
    )(
        *map(
            in_hbm,
            (
                lengths.reshape(1, seq_count),
                tokens,
                mix_gain.reshape(1, width),
                expert_gain.reshape(1, width),
                forget_weight.T,
                routes.T,
                query_weight,
                key_weight,
                value_weight,
                out_weight,
                key_cache,
                value_cache,
                gate_cache,
            ),
        ),
    )
    other_out = lax.ppermute(partial_out, "tp", swap)

    outgoing, own_half = pl.pallas_call(
        dispatch_kernel,
        name="dispatch",
        cost_estimate=pl.CostEstimate(
            flops=COVER, transcendentals=seq_count, bytes_accessed=8 * tokens.size
        ),
        out_shape=(
            jax.ShapeDtypeStruct((rows, quarter), bf16),
            jax.ShapeDtypeStruct((seq_count, columns), bf16),
        ),
        in_specs=[VMEM_SPEC] * 5,
        out_specs=(VMEM_SPEC, VMEM_SPEC),
        scratch_shapes=[
            pltpu.VMEM((seq_count, width), bf16),
            pltpu.VMEM((seq_count, width), bf16),
        ],
        compiler_params=pltpu.CompilerParams(vmem_limit_bytes=6 << 20),
    )(tokens_out, partial_out, other_out, gain_out, slots)

    received = lax.all_to_all(
        outgoing.reshape(chips, 2 * CAP, quarter), "ep", split_axis=0, concat_axis=0, tiled=True
    )
    others = lax.ppermute(received, "tp", swap)

    units = expert_gate.shape[1]
    parts = max(1, units // 512)
    in_rows = chips * CAP
    gate_v, up_v, down_v = in_vmem(expert_gate), in_vmem(expert_up), in_vmem(expert_down)
    expert_params = pltpu.CompilerParams(vmem_limit_bytes=(3 << 20) + 8 * in_rows * width)
    partial = pl.pallas_call(
        functools.partial(first_kernel, parts),
        name="first",
        cost_estimate=pl.CostEstimate(
            flops=2 * in_rows * width * units, transcendentals=0, bytes_accessed=2 * expert_up.size
        ),
        out_shape=pltpu.VMEM((2, in_rows, units), f32),
        in_specs=[VMEM_SPEC] * 3,
        out_specs=VMEM_SPEC,
        scratch_shapes=[pltpu.VMEM((in_rows, columns), bf16)],
        compiler_params=expert_params,
    )(received.reshape(rows, quarter), gate_v, up_v)
    hidden, back_others = pl.pallas_call(
        functools.partial(second_kernel, parts),
        name="second",
        out_shape=(pltpu.VMEM((in_rows, units), bf16), pltpu.VMEM((rows, quarter), bf16)),
        in_specs=[VMEM_SPEC] * 5,
        out_specs=(VMEM_SPEC, VMEM_SPEC),
        scratch_shapes=[pltpu.VMEM((in_rows, columns), bf16)],
        compiler_params=expert_params,
    )(others.reshape(rows, quarter), partial, gate_v, up_v, down_v)
    back_mine = pl.pallas_call(
        third_kernel,
        name="third",
        cost_estimate=pl.CostEstimate(
            flops=in_rows * width * units, transcendentals=0, bytes_accessed=expert_up.size
        ),
        out_shape=pltpu.VMEM((rows, quarter), bf16),
        in_specs=[VMEM_SPEC] * 2,
        out_specs=VMEM_SPEC,
        compiler_params=expert_params,
    )(hidden, down_v)
    from_other = lax.ppermute(back_others, "tp", swap)
    share = (back_mine.astype(f32) + from_other.astype(f32)).astype(bf16)
    returned = lax.all_to_all(
        share.reshape(chips, 2 * CAP, quarter), "ep", split_axis=0, concat_axis=0, tiled=True
    )
    half = pl.pallas_call(
        combine_kernel,
        name="combine",
        out_shape=pltpu.VMEM((seq_count, columns), bf16),
        in_specs=[VMEM_SPEC] * 4,
        out_specs=VMEM_SPEC,
        compiler_params=pltpu.CompilerParams(vmem_limit_bytes=6 << 20),
    )(returned.reshape(rows, quarter), slots, own_half, route_weights.T)
    other_half = lax.ppermute(half, "tp", swap)
    return pl.pallas_call(
        join_kernel,
        name="join",
        out_shape=jax.ShapeDtypeStruct((seq_count, width), bf16),
        in_specs=[VMEM_SPEC] * 2,
        out_specs=HBM_SPEC,
        scratch_shapes=[dma((2,))],
        compiler_params=pltpu.CompilerParams(vmem_limit_bytes=1 << 20),
    )(half, other_half)


def solution(mesh):
    return jax.shard_map(
        on_device,
        mesh=mesh,
        in_specs=(
            P("ep", None),
            P("ep"),
            P("ep", None, "tp"),
            P("ep", None, "tp"),
            P("ep", "tp", None),
            P(),
            P(None, "tp"),
            P(None, "tp"),
            P(None, "tp"),
            P(None, "tp"),
            P("tp", None),
            P(),
            P("ep", None),
            P("ep", None),
            P(None, ("ep", "tp")),
            P(None, ("ep", "tp")),
            P(("ep", "tp"), None),
        ),
        out_specs=P("ep", None),
        check_vma=False,
    )
```

```python
import functools

import jax
import jax.numpy as jnp
from jax import lax
from jax.experimental import pallas as pl
from jax.experimental.pallas import tpu as pltpu
from jax.sharding import PartitionSpec as P

HD = 64
EXPERTS = 8
CAP = 12
LANES = 128
GROUP = 8
STEP = 128
COVER = 10**12

eps = 1e-06
f32 = jnp.float32
bf16 = jnp.bfloat16
VMEM_SPEC = pl.BlockSpec(memory_space=pltpu.VMEM)
HBM_SPEC = pl.BlockSpec(memory_space=pltpu.HBM)
NT = (((1,), (1,)), ((), ()))
TN = (((0,), (0,)), ((), ()))


def in_hbm(array):
    return pltpu.with_memory_space_constraint(array, pltpu.HBM)


def in_vmem(array):
    return pltpu.with_memory_space_constraint(array, pltpu.VMEM)


def iota(shape, dim):
    return lax.broadcasted_iota(jnp.int32, shape, dim)


def quotient(values, divisor):
    return jnp.floor((values.astype(f32) + 0.5) * (1.0 / divisor))


def normed(values, gain):
    floats = values.astype(f32)
    return floats * lax.rsqrt(jnp.mean(floats * floats, axis=-1, keepdims=True) + eps) * gain


def slot_matrix(routes, rows, pieces):
    count = routes.shape[1]
    first, second = routes[0:1, :], routes[1:2, :]
    expert = iota((EXPERTS, count), 0)
    named = ((first == expert) | (second == expert)).astype(f32).astype(bf16)
    earlier = (iota((count, count), 0) < iota((count, count), 1)).astype(f32).astype(bf16)
    slot = jnp.dot(named, earlier, preferred_element_type=f32) + (expert * CAP).astype(f32)
    place0 = jnp.sum(jnp.where(first == expert, slot, 0.0), axis=0, keepdims=True)
    place1 = jnp.sum(jnp.where(second == expert, slot, 0.0), axis=0, keepdims=True)
    unused = jnp.full((1, 2 * count), -1.0, f32)
    lower = jnp.concatenate([place0, place1, unused], axis=1)
    upper = jnp.concatenate([unused, place0, place1], axis=1)
    row = iota((rows, 4 * count), 0)
    block = quotient(row, 2 * CAP)
    within = row.astype(f32) - block * (2 * CAP)
    half = within >= CAP
    wanted = quotient(block, pieces) * CAP + jnp.where(half, within - CAP, within)
    hit = jnp.where(half, (wanted == upper).astype(f32), (wanted == lower).astype(f32))
    return hit.astype(bf16)


def sort_table(row):
    count = row.shape[1]
    lane, sub = iota((count, count), 1), iota((count, count), 0)
    column = jnp.sum(jnp.where(lane == sub, row, 0), axis=1, keepdims=True)
    before = (row < column) | ((row == column) & (lane < sub))
    rank = jnp.sum(before.astype(f32), axis=1, keepdims=True)
    lane, sub = iota((count, LANES), 1), iota((count, LANES), 0)
    hit = rank == lane.astype(f32)
    order = jnp.sum(jnp.where(hit, sub, 0), axis=0, keepdims=True)
    length = jnp.sum(jnp.where(hit, column, 0), axis=0, keepdims=True)
    return order, length


def attention_kernel(
    pieces,
    lengths,
    tokens,
    gain,
    second_gain,
    forget,
    routes,
    wq,
    wk,
    wv,
    wo,
    keys,
    values,
    gates,
    partial_out,
    slots,
    tokens_v,
    second_gain_v,
    lengths_v,
    table_v,
    table_s,
    gain_v,
    forget_v,
    routes_v,
    wq_v,
    wk_v,
    wv_v,
    wo_v,
    keys_v,
    values_v,
    gates_v,
    query_v,
    key_new_v,
    value_new_v,
    log_gate_v,
    mixed_v,
    small_sem,
    weight_sem,
    base_sem,
    key_sem,
    value_sem,
):
    seq_count, positions, _ = keys.shape
    heads = gates.shape[1]
    pairs = heads // 2
    groups = seq_count // GROUP

    small = [
        pltpu.make_async_copy(src, dst, small_sem.at[i])
        for i, (src, dst) in enumerate(
            (
                (lengths, lengths_v),
                (tokens, tokens_v),
                (gain, gain_v),
                (forget, forget_v),
                (routes, routes_v),
                (second_gain, second_gain_v),
            )
        )
    ]
    table_copy = pltpu.make_async_copy(table_v, table_s, small_sem.at[6])
    copies = [
        pltpu.make_async_copy(src, dst, weight_sem.at[i])
        for i, (src, dst) in enumerate(((wq, wq_v), (wk, wk_v), (wv, wv_v), (wo, wo_v)))
    ]

    every = pl.ds(0, seq_count)
    base = pl.ds(0, STEP)
    gate_copy = pltpu.make_async_copy(gates, gates_v, base_sem.at[0])
    key_base = pltpu.make_async_copy(keys.at[every, base], keys_v.at[every, base], base_sem.at[1])
    value_base = pltpu.make_async_copy(
        values.at[every, base], values_v.at[every, base], base_sem.at[2]
    )

    def chunks(g):
        return (table_s[1, g * GROUP + GROUP - 1] + STEP - 1) // STEP

    def group_copies(g):
        window = pl.ds(STEP, pl.multiple_of((chunks(g) - 1) * STEP, STEP))
        pairs_of = []
        for j in range(GROUP):
            s = table_s[0, g * GROUP + j]
            pairs_of.append(
                (
                    pltpu.make_async_copy(keys.at[s, window], keys_v.at[s, window], key_sem.at[s]),
                    pltpu.make_async_copy(
                        values.at[s, window], values_v.at[s, window], value_sem.at[s]
                    ),
                )
            )
        return pairs_of

    for c in small + copies[:3] + [gate_copy, key_base, value_base]:
        c.start()
    small[0].wait()
    order, length = sort_table(lengths_v[...])
    table_v[0:1, :] = order
    table_v[1:2, :] = length
    table_copy.start()
    table_copy.wait()

    def start_group(g, _):
        @pl.when(chunks(g) > 1)
        def _():
            copies_of = group_copies(g)
            for key_copy, _ in copies_of:
                key_copy.start()
            for _, value_copy in copies_of:
                value_copy.start()

        return 0

    lax.fori_loop(0, groups, start_group, 0)
    copies[3].start()

    for c in small[1:]:
        c.wait()
    normal_in = normed(tokens_v[...], gain_v[...]).astype(bf16)
    gate_in = lax.dot_general(forget_v[...], normal_in, NT, preferred_element_type=f32)
    log_gate_v[:, :seq_count] = jnp.minimum(gate_in, 0.0) - jnp.log1p(jnp.exp(-jnp.abs(gate_in)))
    slots[...] = slot_matrix(routes_v[...], slots.shape[0], pieces)
    low = iota((seq_count, LANES), 1) < HD
    for c in copies[:3]:
        c.wait()
    query = jnp.dot(normal_in, wq_v[...], preferred_element_type=f32).astype(bf16).astype(f32)
    query = query * (HD**-0.5)
    key_new_v[...] = (
        jnp.dot(normal_in, wk_v[...], preferred_element_type=f32).astype(bf16).astype(f32)
    )
    value_new_v[...] = (
        jnp.dot(normal_in, wv_v[...], preferred_element_type=f32).astype(bf16).astype(f32)
    )
    for j in range(pairs):
        val = query[:, j * LANES : (j + 1) * LANES]
        turned = pltpu.roll(val, HD, 1)
        if j < pairs // 2:
            one, two = jnp.where(low, val, 0.0), jnp.where(low, turned, 0.0)
        else:
            one, two = jnp.where(low, 0.0, turned), jnp.where(low, 0.0, val)
        query_v[:, 2 * j, :] = one
        query_v[:, 2 * j + 1, :] = two

    lane = iota((heads, LANES), 1)

    def attend(g, reach):
        position = iota((heads, reach), 1)
        scored = []
        for j in range(GROUP):
            i = g * GROUP + j
            s, length = table_s[0, i], table_s[1, i]
            query_s = query_v[s]
            score = lax.dot_general(
                query_s.astype(bf16), keys_v[s, :reach], NT, preferred_element_type=f32
            )
            last = length - 1
            start = pl.multiple_of(last // LANES * LANES, LANES)
            near = gates_v[s, :, pl.ds(start, LANES)]
            picked = jnp.where(lane == last - start, near, 0.0) + jnp.where(
                lane == s, log_gate_v[...], 0.0
            )
            offset = jnp.sum(picked, axis=1, keepdims=True)
            own = jnp.sum(query_s * key_new_v[pl.ds(s, 1), :], axis=1, keepdims=True)
            score = jnp.where(position < length, score + offset - gates_v[s, :, :reach], -jnp.inf)
            highest = jnp.maximum(jnp.max(score, axis=1, keepdims=True), own)
            raised = jnp.exp(score - highest)
            own_raised = jnp.exp(own - highest)
            total = jnp.sum(raised, axis=1, keepdims=True) + own_raised
            scored.append((s, raised.astype(bf16), own_raised, total))
        for j in range(GROUP):
            s, raised, own_raised, total = scored[j]
            product = jnp.dot(raised, values_v[s, :reach], preferred_element_type=f32)
            product = product + own_raised * value_new_v[pl.ds(s, 1), :]
            mixed_v[s] = product / total

    for c in (gate_copy, key_base, value_base):
        c.wait()

    def group_step(g, _):
        count = chunks(g)

        @pl.when(count > 1)
        def _():
            for key_copy, value_copy in group_copies(g):
                key_copy.wait()
                value_copy.wait()

        for n in range(1, positions // STEP + 1):
            pl.when(count == n)(functools.partial(attend, g, n * STEP))
        return 0

    lax.fori_loop(0, groups, group_step, 0)

    parts = []
    for j in range(pairs):
        one, two = mixed_v[:, 2 * j, :], mixed_v[:, 2 * j + 1, :]
        if j < pairs // 2:
            parts.append(jnp.where(low, one, pltpu.roll(two, HD, 1)))
        else:
            parts.append(jnp.where(low, pltpu.roll(one, HD, 1), two))
    mixed = jnp.concatenate(parts, axis=1).astype(bf16)
    copies[3].wait()
    partial_out[...] = jnp.dot(mixed, wo_v[...], preferred_element_type=f32).astype(bf16)


def dispatch_kernel(tokens, own, other, gain, slots, outgoing, own_half, normal_v, full_v):
    columns = own_half.shape[1]
    quarter = columns // 2
    residual = tokens[...].astype(f32) + own[...].astype(f32) + other[...].astype(f32)
    residual = residual.astype(bf16)
    full_v[...] = residual
    normal_v[...] = normed(residual, gain[...]).astype(bf16)
    start = pl.multiple_of(lax.axis_index("tp") * columns, columns)
    own_half[...] = full_v[:, pl.ds(start, columns)]
    first = normal_v[:, pl.ds(start, quarter)]
    second = normal_v[:, pl.ds(pl.multiple_of(start + quarter, quarter), quarter)]
    stacked = jnp.concatenate([first, first, second, second], axis=0)
    outgoing[...] = jnp.dot(slots[...], stacked, preferred_element_type=f32).astype(bf16)


def gather_matrix(rows_in, rows_out, half, turned):
    shape = (rows_in, rows_out) if turned else (rows_out, rows_in)
    dim = 1 if turned else 0
    row = iota(shape, dim)
    source = quotient(row, CAP)
    target = source * (2 * CAP) + half * CAP + (row.astype(f32) - source * CAP)
    return (target == iota(shape, 1 - dim).astype(f32)).astype(f32).astype(bf16)


def unpack_rows(source, rows_v):
    quarter = source.shape[1]
    rows_in = source.shape[0]
    span = min(rows_in, 16 * 2 * CAP)
    for half in range(2):
        matrix = gather_matrix(span, span // 2, half, False)
        for piece in range(rows_in // span):
            rows_v[
                piece * (span // 2) : (piece + 1) * (span // 2),
                half * quarter : (half + 1) * quarter,
            ] = jnp.dot(
                matrix, source[piece * span : (piece + 1) * span, :], preferred_element_type=f32
            ).astype(bf16)


def down_rows(hidden, w_down, target, side, quarter):
    rows_in = target.shape[0]
    span = min(rows_in, 16 * 2 * CAP)
    results = []
    for half in range(2):
        start = pl.multiple_of(side * 2 * quarter + half * quarter, quarter)
        results.append(
            jnp.dot(
                hidden[...], w_down[:, pl.ds(start, quarter)], preferred_element_type=f32
            ).astype(bf16)
        )
    spread = [gather_matrix(span, span // 2, half, True) for half in range(2)]
    for piece in range(rows_in // span):
        taken = slice(piece * (span // 2), (piece + 1) * (span // 2))
        target[piece * span : (piece + 1) * span, :] = (
            jnp.dot(spread[0], results[0][taken], preferred_element_type=f32)
            + jnp.dot(spread[1], results[1][taken], preferred_element_type=f32)
        ).astype(bf16)


def first_kernel(parts, mine, w_gate, w_up, partial, rows_v):
    units = w_gate.shape[1]
    columns = rows_v.shape[1]
    block = units // parts
    rows = pl.ds(pl.multiple_of(lax.axis_index("tp") * columns, columns), columns)
    unpack_rows(mine, rows_v)
    for j in range(parts):
        window = slice(j * block, (j + 1) * block)
        for k, weight in enumerate((w_gate, w_up)):
            partial[k, :, window] = jnp.dot(
                rows_v[...], weight[rows, window], preferred_element_type=f32
            )


def second_kernel(
    parts, others, partial, w_gate, w_up, w_down, hidden_out, out_others, rows_v
):
    units = w_gate.shape[1]
    columns = rows_v.shape[1]
    block = units // parts
    side = 1 - lax.axis_index("tp")
    rows = pl.ds(pl.multiple_of(side * columns, columns), columns)
    unpack_rows(others, rows_v)
    for j in range(parts):
        window = slice(j * block, (j + 1) * block)
        gate_out, up_out = [
            partial[k, :, window]
            + jnp.dot(rows_v[...], weight[rows, window], preferred_element_type=f32)
            for k, weight in enumerate((w_gate, w_up))
        ]
        hidden = gate_out * jax.nn.sigmoid(gate_out) * up_out
        hidden_out[:, window] = hidden.astype(bf16)
    down_rows(hidden_out, w_down, out_others, side, others.shape[1])


def third_kernel(hidden, w_down, out_mine):
    down_rows(hidden, w_down, out_mine, lax.axis_index("tp"), out_mine.shape[1])


def combine_kernel(returned, slots, own_half, route_weights, out):
    seq_count = own_half.shape[0]
    quarter = returned.shape[1]
    picked = lax.dot_general(slots[...], returned[...], TN, preferred_element_type=f32)
    square = iota((seq_count, seq_count), 0) == iota((seq_count, seq_count), 1)
    weights = [
        jnp.sum(jnp.where(square, route_weights[k : k + 1, :], 0.0), axis=1, keepdims=True)
        for k in range(2)
    ]
    for half in range(2):
        base = half * 2 * seq_count
        mixture = picked[base : base + seq_count] * weights[0]
        mixture = mixture + picked[base + seq_count : base + 2 * seq_count] * weights[1]
        span = slice(half * quarter, (half + 1) * quarter)
        out[:, span] = (own_half[:, span].astype(f32) + mixture).astype(bf16)


def join_kernel(half, other, out, sem):
    columns = half.shape[1]
    me = lax.axis_index("tp")
    copies = [
        pltpu.make_async_copy(
            source,
            out.at[:, pl.ds(pl.multiple_of(side * columns, columns), columns)],
            sem.at[i],
        )
        for i, (source, side) in enumerate(((half, me), (other, 1 - me)))
    ]
    for c in copies:
        c.start()
    for c in copies:
        c.wait()


def on_device(
    tokens,
    lengths,
    key_cache,
    value_cache,
    gate_cache,
    mix_gain,
    query_weight,
    key_weight,
    value_weight,
    forget_weight,
    out_weight,
    expert_gain,
    routes,
    route_weights,
    expert_gate,
    expert_up,
    expert_down,
):
    seq_count, width = tokens.shape
    positions = key_cache.shape[1]
    heads = gate_cache.shape[1]
    chips = lax.axis_size("ep")
    pieces = chips // EXPERTS
    rows = chips * 2 * CAP
    columns = width // 2
    quarter = columns // 2
    swap = [(0, 1), (1, 0)]
    dma = pltpu.SemaphoreType.DMA

    partial_out, slots, tokens_out, gain_out = pl.pallas_call(
        functools.partial(attention_kernel, pieces),
        name="attention",
        out_shape=(
            pltpu.VMEM((seq_count, width), bf16),
            pltpu.VMEM((rows, 4 * seq_count), bf16),
            pltpu.VMEM((seq_count, width), bf16),
            pltpu.VMEM((1, width), f32),
        ),
        in_specs=[HBM_SPEC] * 13,
        out_specs=(VMEM_SPEC,) * 4,
        scratch_shapes=[
            pltpu.VMEM((1, seq_count), jnp.int32),
            pltpu.VMEM((2, LANES), jnp.int32),
            pltpu.SMEM((2, LANES), jnp.int32),
            pltpu.VMEM((1, width), f32),
            pltpu.VMEM((heads, width), bf16),
            pltpu.VMEM((2, seq_count), jnp.int32),
            pltpu.VMEM(query_weight.shape, bf16),
            pltpu.VMEM(key_weight.shape, bf16),
            pltpu.VMEM(value_weight.shape, bf16),
            pltpu.VMEM(out_weight.shape, bf16),
            pltpu.VMEM(key_cache.shape, bf16),
            pltpu.VMEM(value_cache.shape, bf16),
            pltpu.VMEM(gate_cache.shape, f32),
            pltpu.VMEM((seq_count, heads, LANES), f32),
            pltpu.VMEM((seq_count, LANES), f32),
            pltpu.VMEM((seq_count, LANES), f32),
            pltpu.VMEM((heads, LANES), f32),
            pltpu.VMEM((seq_count, heads, LANES), f32),
            dma((7,)),
            dma((4,)),
            dma((3,)),
            dma((seq_count,)),
            dma((seq_count,)),
        ],
        compiler_params=pltpu.CompilerParams(vmem_limit_bytes=59 << 20),
    )(
        *map(
            in_hbm,
            (
                lengths.reshape(1, seq_count),
                tokens,
                mix_gain.reshape(1, width),
                expert_gain.reshape(1, width),
                forget_weight.T,
                routes.T,
                query_weight,
                key_weight,
                value_weight,
                out_weight,
                key_cache,
                value_cache,
                gate_cache,
            ),
        ),
    )
    other_out = lax.ppermute(partial_out, "tp", swap)

    outgoing, own_half = pl.pallas_call(
        dispatch_kernel,
        name="dispatch",
        cost_estimate=pl.CostEstimate(
            flops=COVER, transcendentals=seq_count, bytes_accessed=8 * tokens.size
        ),
        out_shape=(
            jax.ShapeDtypeStruct((rows, quarter), bf16),
            jax.ShapeDtypeStruct((seq_count, columns), bf16),
        ),
        in_specs=[VMEM_SPEC] * 5,
        out_specs=(VMEM_SPEC, VMEM_SPEC),
        scratch_shapes=[
            pltpu.VMEM((seq_count, width), bf16),
            pltpu.VMEM((seq_count, width), bf16),
        ],
        compiler_params=pltpu.CompilerParams(vmem_limit_bytes=6 << 20),
    )(tokens_out, partial_out, other_out, gain_out, slots)

    received = lax.all_to_all(
        outgoing.reshape(chips, 2 * CAP, quarter), "ep", split_axis=0, concat_axis=0, tiled=True
    )
    others = lax.ppermute(received, "tp", swap)

    units = expert_gate.shape[1]
    parts = max(1, units // 512)
    in_rows = chips * CAP
    gate_v, up_v, down_v = in_vmem(expert_gate), in_vmem(expert_up), in_vmem(expert_down)
    expert_params = pltpu.CompilerParams(vmem_limit_bytes=(3 << 20) + 8 * in_rows * width)
    partial = pl.pallas_call(
        functools.partial(first_kernel, parts),
        name="first",
        cost_estimate=pl.CostEstimate(
            flops=2 * in_rows * width * units, transcendentals=0, bytes_accessed=2 * expert_up.size
        ),
        out_shape=pltpu.VMEM((2, in_rows, units), f32),
        in_specs=[VMEM_SPEC] * 3,
        out_specs=VMEM_SPEC,
        scratch_shapes=[pltpu.VMEM((in_rows, columns), bf16)],
        compiler_params=expert_params,
    )(received.reshape(rows, quarter), gate_v, up_v)
    hidden, back_others = pl.pallas_call(
        functools.partial(second_kernel, parts),
        name="second",
        out_shape=(pltpu.VMEM((in_rows, units), bf16), pltpu.VMEM((rows, quarter), bf16)),
        in_specs=[VMEM_SPEC] * 5,
        out_specs=(VMEM_SPEC, VMEM_SPEC),
        scratch_shapes=[pltpu.VMEM((in_rows, columns), bf16)],
        compiler_params=expert_params,
    )(others.reshape(rows, quarter), partial, gate_v, up_v, down_v)
    back_mine = pl.pallas_call(
        third_kernel,
        name="third",
        cost_estimate=pl.CostEstimate(
            flops=in_rows * width * units, transcendentals=0, bytes_accessed=expert_up.size
        ),
        out_shape=pltpu.VMEM((rows, quarter), bf16),
        in_specs=[VMEM_SPEC] * 2,
        out_specs=VMEM_SPEC,
        compiler_params=expert_params,
    )(hidden, down_v)
    from_other = lax.ppermute(back_others, "tp", swap)
    share = (back_mine.astype(f32) + from_other.astype(f32)).astype(bf16)
    returned = lax.all_to_all(
        share.reshape(chips, 2 * CAP, quarter), "ep", split_axis=0, concat_axis=0, tiled=True
    )
    half = pl.pallas_call(
        combine_kernel,
        name="combine",
        out_shape=pltpu.VMEM((seq_count, columns), bf16),
        in_specs=[VMEM_SPEC] * 4,
        out_specs=VMEM_SPEC,
        compiler_params=pltpu.CompilerParams(vmem_limit_bytes=6 << 20),
    )(returned.reshape(rows, quarter), slots, own_half, route_weights.T)
    other_half = lax.ppermute(half, "tp", swap)
    return pl.pallas_call(
        join_kernel,
        name="join",
        out_shape=jax.ShapeDtypeStruct((seq_count, width), bf16),
        in_specs=[VMEM_SPEC] * 2,
        out_specs=HBM_SPEC,
        scratch_shapes=[dma((2,))],
        compiler_params=pltpu.CompilerParams(vmem_limit_bytes=1 << 20),
    )(half, other_half)


def solution(mesh):
    return jax.shard_map(
        on_device,
        mesh=mesh,
        in_specs=(
            P("ep", None),
            P("ep"),
            P("ep", None, "tp"),
            P("ep", None, "tp"),
            P("ep", "tp", None),
            P(),
            P(None, "tp"),
            P(None, "tp"),
            P(None, "tp"),
            P(None, "tp"),
            P("tp", None),
            P(),
            P("ep", None),
            P("ep", None),
            P(None, ("ep", "tp")),
            P(None, ("ep", "tp")),
            P(("ep", "tp"), None),
        ),
        out_specs=P("ep", None),
        check_vma=False,
    )
```
